256 devices in a mesh: ep: 64 (over z, y, core), tp: 4 (over x).
Axes of the slice: x: 4, y: 4, z: 8, core: 2. Of those that a mesh axis runs over, the one named last changes fastest.
Arguments:
- glu_value: bfloat16 [32768, 1024], P('ep', 'tp'), may hold values from -6 to 6
- glu_gate: bfloat16 [32768, 1024], P('ep', 'tp'), may hold values from -12 to 12
- conv_kernel: float32 [31, 1024], P(None, 'tp'), may hold values from -11.49474 to 11.49474
- ln_gain: float32 [1024], P('tp'), may hold values from 0.1 to 1.9
- out_weight: bfloat16 [1024, 2048], P('tp'), may hold values from -0.1875 to 0.1875
- moe_input: bfloat16 [16384, 2048], P('ep'), may hold values from -6 to 6
- moe_gain: float32 [2048], replicated, may hold values from 0.1 to 1.9
- gate_weight: bfloat16 [64, 2048, 3072], P('ep', None, 'tp'), may hold values from -0.125 to 0.125
- up_weight: bfloat16 [64, 2048, 3072], P('ep', None, 'tp'), may hold values from -0.125 to 0.125
- down_weight: bfloat16 [64, 3072, 2048], P('ep', 'tp'), may hold values from -0.109375 to 0.109375
- expert_ids: int32 [16384, 2], P('ep'), may hold values from 0 to 63, all different within a row; in each aligned block of 256 rows (0 to 255, 256 to 511, ...) at most 16 rows name the same one
- route_weight: float32 [16384, 2], P('ep'), may hold values from 0.2 to 1
Outputs:
- mixer_out: bfloat16 [32768, 2048], P(('ep', 'tp'))
- expert_out: bfloat16 [16384, 2048], P('ep', 'tp')
The draws below stay inside these ranges and needn't reach their ends.
Inputs may be any that keep to these rules, and one draw needn't show every extreme that they name: `expert_ids`: each row names 2 different experts. In the rows of one device no expert is named by more than 16 rows; the bound is reached at some expert in some device's rows.
All inputs are finite; a program needn't handle non-finite values.
Results may differ from the reference program's by a relative error of at most 0.012.
Values may be sent and summed in bfloat16 or wider, within the bound.
No kernel may reach another device: no remote copies, remote signals or barrier semaphores. Data moves between devices by JAX's collectives and lax.ppermute only.
A program may use at most 64 MiB of HBM per device.

```python
import math
import jax
import jax.numpy as jnp
import numpy as np
from jax import lax

D = 2048
MIX = 1024
KERNEL = 31
FF = 3072
TOP = 2
TOKB_DEV = 256
EXPERTS = 64
CAP = 16
TOKA = 32768
TOKB = 16384
N_EP = 64
N_TP = 4


def draw_conv_kernel(key, part):
    base_key = jax.random.fold_in(key, 17)
    rough_key = jax.random.fold_in(key, 29)
    position = jnp.arange(MIX, dtype=jnp.float32) / MIX
    rough = jnp.exp(jax.random.uniform(rough_key, (MIX,), jnp.float32, math.log(0.6), math.log(1.6)))
    scale = jnp.exp(position * math.log(10.0)) * rough * KERNEL ** (-0.5)
    base = jnp.clip(jax.random.normal(base_key, (KERNEL, MIX), jnp.float32), -4.0, 4.0)
    return (base * scale[None, :]).astype(jnp.float32)


def level_of(key, shape, shards, low, high):
    def one(axis_at, shards_of):
        heights = jax.random.uniform(jax.random.fold_in(jax.random.fold_in(key, 6), axis_at), (shards_of,), jnp.float32, low / len(shards), high / len(shards))
        return jnp.repeat(jnp.exp(heights), shape[axis_at] // shards_of).reshape((-1,) + (1,) * (len(shape) - axis_at - 1))

    level = one(*shards[0])
    for cut in shards[1:]:
        level = level * one(*cut)
    return level


def shared_out(key, own, number, rows, number_of, top, reach, skew):
    ranking = jax.random.permutation(key, number_of)
    crowded, ordinary = load_shares(number_of, rows * top, reach, skew, True), load_shares(number_of, rows * top, reach, skew, False)
    places = jnp.arange(number_of)

    def named(tallies, offset_by):
        used = int((tallies > 0).sum())
        fixed = max(1, used // 4)
        moved = fixed + (places - fixed + offset_by * (used - fixed)) % max(1, number_of - fixed)
        return jnp.zeros((number_of,), jnp.int32).at[ranking[jnp.where(places < fixed, places, moved)]].set(jnp.asarray(tallies, jnp.int32))

    tallies = jnp.where(number % 4 == 0, named(crowded, number // 4), named(ordinary, number - number // 4 - 1))
    mixed = jax.random.permutation(jax.random.fold_in(own, 3), number_of)
    donor, receiver = mixed[0:number_of // 2 * 2:2], mixed[1:number_of // 2 * 2:2]
    margin = jnp.minimum(tallies[donor] - 1, reach - tallies[receiver]) // 2
    margin = jnp.where((donor == ranking[0]) | (receiver == ranking[0]) | (tallies[receiver] == 0), 0, jnp.maximum(margin, 0))
    moved = jax.random.randint(jax.random.fold_in(own, 4), (number_of // 2,), 0, 1 << 20) % (margin + 1)
    tallies = tallies.at[donor].add(-moved).at[receiver].add(moved)
    members = jnp.searchsorted(jnp.cumsum(tallies), jnp.arange(rows * top), side="right").astype(jnp.int32)
    grid = members.reshape(top, rows).T
    grid = grid[jax.random.permutation(jax.random.fold_in(own, 1), rows)]
    offset_by = jax.random.randint(jax.random.fold_in(own, 2), (rows, 1), 0, top)
    return jnp.take_along_axis(grid, (jnp.arange(top)[None, :] + offset_by) % top, axis=1)


def load_shares(number_of, total, most, skew, full):
    portions = [(1 << 20) // math.isqrt(rank ** skew) + 1 for rank in range(1, number_of + 1)]
    largest = most if full else min(most, max(-(-total // number_of), total * portions[0] // sum(portions)))
    least = 1 if total - largest >= number_of - 1 else 0
    counts, rest = [largest] + [least] * (number_of - 1), total - largest - least * (number_of - 1)
    while rest > 0:
        movable = [i for i in range(1, number_of) if counts[i] < largest] or [i for i in range(1, number_of) if counts[i] < most]
        pool, budget = sum([portions[i] for i in movable]), rest
        for i in movable:
            extra = min(most - counts[i], max(1, budget * portions[i] // pool), rest)
            counts[i] = counts[i] + extra
            rest = rest - extra
    return np.array(counts)


def normal_values(key, shape, scale, limit, pieces=(), kind=jnp.bfloat16):
    entries = scale * jax.random.normal(key, shape, jnp.float32)
    if pieces:
        entries = entries * level_of(key, shape, pieces, -0.22, 0.18)
    return jnp.clip(entries, -limit, limit).astype(kind)


def setup_inputs(seed: int = 0) -> dict:
    streams_of = jax.random.split(jax.random.key(seed), 13)
    glu_value = normal_values(streams_of[0], (TOKA, MIX), 1.0, 6.0, ((0, 64), (1, 4)))
    glu_gate = normal_values(streams_of[1], (TOKA, MIX), 2.0, 12.0, ((0, 64), (1, 4)))
    conv_kernel = draw_conv_kernel(jax.random.fold_in(streams_of[12], 71), 0)
    ln_gain = jnp.clip(1.0 + 0.18 * jax.random.normal(streams_of[3], (MIX,), jnp.float32), 0.1, 1.9)
    out_weight = normal_values(streams_of[4], (MIX, D), MIX ** -0.5, 0.1875, ((0, 4),))
    moe_input = normal_values(streams_of[5], (TOKB, D), 1.0, 6.0, ((0, 64),))
    moe_gain = jnp.clip(1.0 + 0.18 * jax.random.normal(streams_of[6], (D,), jnp.float32), 0.1, 1.9)
    gate_weight = normal_values(streams_of[7], (EXPERTS, D, FF), D ** -0.5, 0.125, ((0, 64), (2, 4)))
    up_weight = normal_values(streams_of[8], (EXPERTS, D, FF), D ** -0.5, 0.125, ((0, 64), (2, 4)))
    down_weight = normal_values(streams_of[9], (EXPERTS, FF, D), FF ** -0.5, 0.109375, ((0, 64), (1, 4)))
    expert_ids_keys = jax.random.split(jax.random.fold_in(streams_of[10], 1), TOKB // TOKB_DEV)
    expert_ids_turns = jax.random.permutation(jax.random.fold_in(streams_of[10], 3), TOKB // TOKB_DEV)
    expert_ids = jax.vmap(lambda own, number: shared_out(jax.random.fold_in(streams_of[10], 2), own, number, TOKB_DEV, EXPERTS, TOP, CAP, 1))(expert_ids_keys, expert_ids_turns).reshape((TOKB, TOP))
    route_weight = jnp.clip(0.2 + 0.8 * jax.random.uniform(streams_of[11], (TOKB, TOP), jnp.float32) ** level_of(streams_of[11], (TOKB, TOP), ((0, 64),), -0.2, 0.2), 0.2, 1.0)
    return {"glu_value": glu_value, "glu_gate": glu_gate, "conv_kernel": conv_kernel, "ln_gain": ln_gain, "out_weight": out_weight, "moe_input": moe_input, "moe_gain": moe_gain, "gate_weight": gate_weight, "up_weight": up_weight, "down_weight": down_weight, "expert_ids": expert_ids, "route_weight": route_weight}


eps_rms = 1e-06
eps_norm = 1e-05

def slot_numbers(expert_ids, experts, capacity):
    chosen = expert_ids.reshape(-1)
    onehot = (chosen[:, None] == jnp.arange(experts, dtype=jnp.int32)[None, :]).astype(jnp.int32)
    earlier = jnp.cumsum(onehot, axis=0) - onehot
    position = lax.optimization_barrier(jnp.sum(earlier * onehot, axis=1))
    return (chosen * capacity + position).astype(jnp.int32)

def fill_slots(normed, slot_index, experts, capacity, chosen_per_token):
    owners = jnp.full((experts * capacity,), -1, jnp.int32)
    token_of = (jnp.arange(slot_index.shape[0], dtype=jnp.int32) // chosen_per_token).astype(jnp.int32)
    owners = owners.at[slot_index].set(token_of)
    picked = jnp.take(normed, jnp.maximum(owners, 0), axis=0)
    filled = jnp.where((owners >= 0)[:, None], picked, jnp.zeros_like(picked))
    return filled.reshape(experts, capacity, normed.shape[1])

def mixer_half(glu_value, glu_gate, conv_kernel, ln_gain, out_weight):
    gated = (glu_value.astype(jnp.float32) * jax.nn.sigmoid(glu_gate.astype(jnp.float32))).astype(jnp.bfloat16)
    length = gated.shape[0]
    padded = jnp.concatenate([jnp.zeros((KERNEL - 1, MIX), jnp.bfloat16), gated], axis=0).astype(jnp.float32)
    convolved = jnp.zeros((length, MIX), jnp.float32)
    for tap_index in range(KERNEL):
        begin = KERNEL - 1 - tap_index
        convolved = convolved + conv_kernel[tap_index] * padded[begin:begin + length]
    total = lax.optimization_barrier(jnp.sum(convolved, axis=1))
    squares = lax.optimization_barrier(jnp.sum(convolved * convolved, axis=1))
    mean = total / MIX
    variance = squares / MIX - mean * mean
    scaled = (convolved - mean[:, None]) * lax.rsqrt(variance + eps_norm)[:, None] * ln_gain
    activated = jax.nn.silu(scaled).astype(jnp.bfloat16)
    group = MIX // N_TP
    result = jnp.zeros((length, D), jnp.float32)
    for part_index in range(N_TP):
        partial_sum = jnp.dot(activated[:, part_index * group:(part_index + 1) * group], out_weight[part_index * group:(part_index + 1) * group], preferred_element_type=jnp.float32).astype(jnp.bfloat16)
        result = result + partial_sum.astype(jnp.float32)
    return result.astype(jnp.bfloat16)

def run_expert(operands):
    arrived, w_gate, w_up, w_down = operands
    gate_act = jnp.dot(arrived, w_gate, preferred_element_type=jnp.float32)
    up_act = jnp.dot(arrived, w_up, preferred_element_type=jnp.float32)
    hidden = (jax.nn.silu(gate_act) * up_act).astype(jnp.bfloat16)
    group = FF // N_TP
    total = jnp.zeros((arrived.shape[0], D), jnp.float32)
    for part_index in range(N_TP):
        partial_sum = jnp.dot(hidden[:, part_index * group:(part_index + 1) * group], w_down[part_index * group:(part_index + 1) * group], preferred_element_type=jnp.float32).astype(jnp.bfloat16)
        total = total + partial_sum.astype(jnp.float32)
    return total.astype(jnp.bfloat16)

def expert_half(moe_input, moe_gain, gate_weight, up_weight, down_weight, expert_ids, route_weight):
    values = moe_input.astype(jnp.float32)
    normed = (values * lax.rsqrt(lax.optimization_barrier(jnp.mean(values * values, axis=1, keepdims=True)) + eps_rms) * moe_gain).astype(jnp.bfloat16)
    normed_blocks = normed.reshape(N_EP, TOKB_DEV, D)
    id_blocks = expert_ids.reshape(N_EP, TOKB_DEV, TOP)
    slot_index = jax.vmap(lambda ids: slot_numbers(ids, EXPERTS, CAP))(id_blocks)
    sent = jax.vmap(lambda block, slots: fill_slots(block, slots, EXPERTS, CAP, TOP))(normed_blocks, slot_index)
    by_expert = jnp.swapaxes(sent, 0, 1).reshape(EXPERTS, N_EP * CAP, D)
    answers = lax.map(run_expert, (by_expert, gate_weight, up_weight, down_weight))
    answers = jnp.swapaxes(answers.reshape(EXPERTS, N_EP, CAP, D), 0, 1).reshape(N_EP, EXPERTS * CAP, D)

    def combine(block_answers, slots, weights):
        picked = jnp.take(block_answers, slots, axis=0).astype(jnp.float32).reshape(TOKB_DEV, TOP, D)
        return lax.optimization_barrier(jnp.sum(picked * weights[:, :, None], axis=1))
    mixed = jax.vmap(combine)(answers, slot_index, route_weight.reshape(N_EP, TOKB_DEV, TOP))
    return mixed.reshape(N_EP * TOKB_DEV, D).astype(jnp.bfloat16)

def reference(glu_value, glu_gate, conv_kernel, ln_gain, out_weight, moe_input, moe_gain, gate_weight, up_weight, down_weight, expert_ids, route_weight):
    mixer_out = mixer_half(glu_value, glu_gate, conv_kernel, ln_gain, out_weight)
    expert_out = expert_half(moe_input, moe_gain, gate_weight, up_weight, down_weight, expert_ids, route_weight)
    return (mixer_out, expert_out)
```

```python
import functools

import jax
import jax.numpy as jnp
from jax import lax
from jax.experimental import pallas as pl
from jax.experimental.pallas import tpu as pltpu
from jax.sharding import PartitionSpec as P


eps_rms = 1e-06
eps_norm = 1e-05
f32 = jnp.float32
bf16 = jnp.bfloat16


VMEM = pl.BlockSpec(memory_space=pltpu.VMEM)
SMEM = pl.BlockSpec(memory_space=pltpu.SMEM)
ANY = pl.BlockSpec(memory_space=pl.ANY)


def dot(a, b):
    return jnp.dot(a, b, preferred_element_type=f32)


def over_tp(value, by):
    count = lax.axis_size("tp")
    return lax.ppermute(value, "tp", [(i, (i + by) % count) for i in range(count)])


def from_behind(value, axis, by):
    count = lax.axis_size(axis)
    return lax.ppermute(value, axis, [(i, i + by) for i in range(count - by)])


def swap_cores(value):
    count = lax.axis_size("ep")
    return lax.ppermute(value, "ep", [(i, i ^ 1) for i in range(count)])


def gather_direct(value):
    return over_tp(value, -1), over_tp(value, 1), over_tp(value, 2)


def gather_relayed(value):
    half = value.shape[0] // 2
    ahead = over_tp(value, -1)
    behind = over_tp(value, 1)
    top = over_tp(ahead[:half], -1)
    bottom = over_tp(behind[half:], 1)
    return ahead, behind, top, bottom


def slot_tables(ids, rows, tokens, per_chunk):
    expert_of = lax.broadcasted_iota(jnp.int32, (rows, tokens), 0) // per_chunk
    first = expert_of == ids[0:1, :]
    second = expert_of == ids[1:2, :]
    chosen = jnp.logical_or(first, second)
    before = (
        lax.broadcasted_iota(jnp.int32, (tokens, tokens), 0)
        < lax.broadcasted_iota(jnp.int32, (tokens, tokens), 1)
    ).astype(f32).astype(bf16)
    earlier = dot(chosen.astype(f32).astype(bf16), before).astype(jnp.int32)
    place = lax.broadcasted_iota(jnp.int32, (rows, tokens), 0) % per_chunk
    return first, second, chosen, earlier, place


def fetch(sources, targets, sems):
    copies = [
        pltpu.make_async_copy(source, target, sems.at[i])
        for i, (source, target) in enumerate(zip(sources, targets))
    ]
    for copy in copies:
        copy.start()
    return copies


def dispatch_kernel(per_chunk, tp_ref, x_hbm, gain_hbm, ids_hbm, o0, o1, x_ref, gain_ref, ids_ref, sems):
    outs = (o0, o1)
    tokens, width = x_ref.shape
    rows, part = o0.shape
    for copy in fetch((x_hbm, gain_hbm, ids_hbm), (x_ref, gain_ref, ids_ref), sems):
        copy.wait()
    squares = jnp.zeros((tokens, 128), f32)
    for begin in range(0, width, 128):
        block = x_ref[:, begin : begin + 128].astype(f32)
        squares = squares + block * block
    scale = lax.rsqrt(jnp.sum(squares, axis=1, keepdims=True) / width + eps_rms)
    start = pl.multiple_of(tp_ref[0] * part, part)
    mine = x_ref[:, pl.ds(start, part)].astype(f32)
    normed = (mine * scale * gain_ref[:, pl.ds(start, part)]).astype(bf16)
    _, _, chosen, earlier, place = slot_tables(ids_ref[...], rows, tokens, per_chunk)
    for chunk, out in enumerate(outs):
        pick = jnp.logical_and(chosen, earlier == place + chunk * per_chunk)
        out[...] = dot(pick.astype(f32).astype(bf16), normed).astype(bf16)


def route_kernel(per_chunk, ids_ref, weight_ref, high_ref, low_ref):
    tokens, slots = high_ref.shape
    rows = slots // 2
    first, second, _, earlier, place = slot_tables(ids_ref[...], rows, tokens, per_chunk)
    amount = jnp.where(first, weight_ref[0:1, :], jnp.where(second, weight_ref[1:2, :], 0.0))
    for chunk in range(2):
        weights = jnp.where(earlier == place + chunk * per_chunk, amount, 0.0).T
        high = weights.astype(bf16)
        high_ref[:, chunk * rows : (chunk + 1) * rows] = high
        low_ref[:, chunk * rows : (chunk + 1) * rows] = (weights - high.astype(f32)).astype(bf16)


def expert_kernel(chunk, tp_ref, own, ahead, behind, *refs):
    if chunk == 0:
        across_in, *refs = refs
    else:
        top, bottom, *refs = refs
    weights, outs, scratch = refs[:3], refs[3:-7], refs[-7:]
    kept, (to_ahead, to_behind, across), sems = scratch[:3], scratch[3:6], scratch[6]
    rows, part = own.shape
    half = rows // 2
    width = weights[0].shape[0]
    count = width // part
    tp = tp_ref[0]
    starts = [
        pl.multiple_of(lax.rem(tp + k, count) * part, part) for k in (0, 1, count - 1, 2)
    ]
    gate_ref, up_ref, down_ref = kept
    sources, targets = [], []
    for start in starts:
        for source, target in zip(weights[:2], kept[:2]):
            sources.append(source.at[pl.ds(start, part), :])
            targets.append(target.at[pl.ds(start, part), :])
    copies = fetch(sources + [weights[2]], targets + [down_ref], sems)
    if chunk == 0:
        to_own, ahead_out, behind_out, across_top, across_bottom = outs
        to_ahead, to_behind = ahead_out, behind_out
        blocks = (own, ahead, behind, across_in)
    else:
        to_own, ahead_top, ahead_bottom, behind_top, behind_bottom, across_top, across_bottom = outs
        across[:half, :] = top[...]
        across[half:, :] = bottom[...]
        blocks = (own, ahead, behind, across)

    def step(i, carry):
        at = pl.ds(pl.multiple_of(i * half, half), half)
        gate = None
        up = None
        for k, (x, start) in enumerate(zip(blocks, starts)):

            @pl.when(i == 0)
            def _():
                copies[2 * k].wait()
                copies[2 * k + 1].wait()

            block = x[at, :]
            g = dot(block, gate_ref[pl.ds(start, part), :])
            u = dot(block, up_ref[pl.ds(start, part), :])
            gate = g if gate is None else gate + g
            up = u if up is None else up + u
        hidden = (jax.nn.silu(gate) * up).astype(bf16)

        @pl.when(i == 0)
        def _():
            copies[-1].wait()

        for out, start in zip((to_own, to_ahead, to_behind, across), starts):
            out[at, :] = dot(hidden, down_ref[:, pl.ds(start, part)]).astype(bf16)
        return carry

    lax.fori_loop(0, 2, step, 0)
    across_top[...] = across[:half, :]
    across_bottom[...] = across[half:, :]
    if chunk == 1:
        ahead_top[...] = to_ahead[:half, :]
        ahead_bottom[...] = to_ahead[half:, :]
        behind_top[...] = to_behind[:half, :]
        behind_bottom[...] = to_behind[half:, :]


def fold_whole_kernel(ahead, top, behind, bottom, ahead_out, behind_out):
    half = top.shape[0]
    ahead_out[:half, :] = (ahead[:half, :].astype(f32) + top[...].astype(f32)).astype(bf16)
    ahead_out[half:, :] = ahead[half:, :]
    behind_out[:half, :] = behind[:half, :]
    behind_out[half:, :] = (behind[half:, :].astype(f32) + bottom[...].astype(f32)).astype(bf16)


def total_whole_kernel(own, first, second, out):
    out[...] = (own[...].astype(f32) + first[...].astype(f32) + second[...].astype(f32)).astype(bf16)


def fold_kernel(a, b, c, d, ab, cd):
    ab[...] = (a[...].astype(f32) + b[...].astype(f32)).astype(bf16)
    cd[...] = (c[...].astype(f32) + d[...].astype(f32)).astype(bf16)


def total_kernel(own, top0, top1, bottom0, bottom1, out):
    half = top0.shape[0]
    out[:half, :] = (
        own[:half, :].astype(f32) + top0[...].astype(f32) + top1[...].astype(f32)
    ).astype(bf16)
    out[half:, :] = (
        own[half:, :].astype(f32) + bottom0[...].astype(f32) + bottom1[...].astype(f32)
    ).astype(bf16)


def conv_kernel_body(reach, halo, b0, b1, b2, b3, out_ref, wide, kept):
    own = out_ref.shape[0]
    part = b0.shape[1]
    channels = 4 * part
    total = jnp.zeros((own, 128), f32)
    square = jnp.zeros((own, 128), f32)
    rows = own + halo
    gains = []
    for k, block in enumerate((b0, b1, b2, b3)):
        taps = sum(
            block[rows + i * (reach + 1) : rows + (i + 1) * (reach + 1), :].astype(f32)
            for i in range(3)
        )
        gains.append(taps[reach : reach + 1, :])
        for begin in range(0, part, 128):
            lanes = slice(begin, begin + 128)
            wide[...] = block[:rows, lanes].astype(f32)
            value = jnp.zeros((own, 128), f32)
            for j in range(reach):
                value = value + taps[j : j + 1, lanes] * wide[halo - j : halo - j + own, :]
            kept[:, k * part + begin : k * part + begin + 128] = value
            total = total + value
            square = square + value * value
    mean = jnp.sum(total, axis=1, keepdims=True) / channels
    variance = jnp.sum(square, axis=1, keepdims=True) / channels - mean * mean
    scale = lax.rsqrt(variance + eps_norm)
    for k in range(4):
        lanes = slice(k * part, (k + 1) * part)
        scaled = (kept[:, lanes] - mean) * scale * gains[k]
        out_ref[:, lanes] = jax.nn.silu(scaled).astype(bf16)


def mix_kernel(core_ref, act, own, n1, n2, n3, far_ref, out_ref):
    part = own.shape[0]
    columns = n1.shape[1]
    core = core_ref[0]
    near_at = pl.ds(pl.multiple_of(core * columns, columns), columns)
    far_at = pl.ds(pl.multiple_of((1 - core) * columns, columns), columns)
    cut = lambda k: act[:, k * part : (k + 1) * part]
    near = dot(cut(0), own[:, near_at]) + dot(cut(1), n1[...])
    near = near + dot(cut(2), n2[...]) + dot(cut(3), n3[...])
    out_ref[:, near_at] = near.astype(bf16)
    far = dot(cut(0), own[:, far_at]) + dot(act[:, part:], far_ref[...])
    out_ref[:, far_at] = far.astype(bf16)


def combine_kernel(high_ref, low_ref, a0_hbm, a1_hbm, out_ref, a0, a1, sems):
    rows = a0.shape[0]
    copies = fetch((a0_hbm, a1_hbm), (a0, a1), sems)
    total = None
    for chunk, (copy, answers) in enumerate(zip(copies, (a0, a1))):
        copy.wait()
        cols = slice(chunk * rows, (chunk + 1) * rows)
        for weights in (high_ref, low_ref):
            term = dot(weights[:, cols], answers[...])
            total = term if total is None else total + term
    out_ref[...] = total.astype(bf16)


def call(kernel, out_shape, in_specs, flops, limit, scratch=()):
    many = isinstance(out_shape, (list, tuple))
    return pl.pallas_call(
        kernel,
        out_shape=out_shape,
        in_specs=in_specs,
        out_specs=[VMEM] * len(out_shape) if many else VMEM,
        scratch_shapes=scratch,
        compiler_params=pltpu.CompilerParams(vmem_limit_bytes=limit * 1024 * 1024),
        cost_estimate=pl.CostEstimate(flops=flops, bytes_accessed=1 << 20, transcendentals=0),
    )


def shape(*dims):
    return jax.ShapeDtypeStruct(dims, bf16)


def split_three(value):
    high = value.astype(bf16)
    rest = value - high.astype(f32)
    middle = rest.astype(bf16)
    return high, middle, (rest - middle.astype(f32)).astype(bf16)


def mixer_half(glu_value, glu_gate, conv_kernel, ln_gain, out_weight):
    tp = lax.axis_index("tp")
    core = lax.axis_index("ep") % 2
    length, part = glu_value.shape
    reach = conv_kernel.shape[0]
    count = lax.axis_size("tp")
    own = length // count
    halo = 32
    columns = out_weight.shape[1] // 2
    mine = lax.dynamic_slice_in_dim(out_weight, core * columns, columns, 1)
    near = gather_direct(mine)
    far = swap_cores(jnp.concatenate(near, axis=0))
    taps = jnp.concatenate([conv_kernel, ln_gain[None, :]], axis=0)
    taps = split_three(taps)
    gated = (glu_value.astype(f32) * jax.nn.sigmoid(glu_gate.astype(f32))).astype(bf16)
    before = from_behind(gated[length - halo :], "ep", 1)
    padded = jnp.concatenate([before, gated], axis=0)

    def rows_of(k):
        rows = lax.dynamic_slice_in_dim(padded, ((tp + k) % count) * own, own + halo, 0)
        return jnp.concatenate([rows, *taps], axis=0)

    blocks = (
        rows_of(0),
        over_tp(rows_of(count - 1), -1),
        over_tp(rows_of(1), 1),
        over_tp(rows_of(2), 2),
    )
    activated = call(
        functools.partial(conv_kernel_body, reach, halo),
        shape(own, part * count),
        [VMEM] * 4,
        10**9,
        8,
        [pltpu.VMEM((own + halo, 128), f32), pltpu.VMEM((own, part * count), f32)],
    )(*blocks)
    return call(
        mix_kernel,
        shape(own, 2 * columns),
        [SMEM] + [VMEM] * 6,
        2 * own * part * count * 2 * columns,
        8,
    )(core.astype(jnp.int32).reshape(1), activated, out_weight, *near, far)


def expert_half(moe_input, moe_gain, gate_weight, up_weight, down_weight, expert_ids, route_weight):
    tokens, width = moe_input.shape
    experts = lax.axis_size("ep")
    count = lax.axis_size("tp")
    capacity = 4 * max(1, tokens // experts)
    chunks = 2
    per_chunk = capacity // chunks
    rows = experts * per_chunk
    half = rows // 2
    part = width // count
    tp = lax.axis_index("tp").astype(jnp.int32).reshape(1)
    ids = expert_ids.T

    def exchange(value):
        value = value.reshape(experts, per_chunk, part)
        moved = lax.all_to_all(value, "ep", split_axis=0, concat_axis=0, tiled=True)
        return moved.reshape(rows, part)

    sent = call(
        functools.partial(dispatch_kernel, per_chunk),
        [shape(rows, part)] * chunks,
        [SMEM, ANY, ANY, ANY],
        2 * 2 * rows * tokens * part,
        56,
        [
            pltpu.VMEM((tokens, width), bf16),
            pltpu.VMEM((1, width), f32),
            pltpu.VMEM(ids.shape, jnp.int32),
            pltpu.SemaphoreType.DMA((3,)),
        ],
    )(tp, moe_input, moe_gain.reshape(1, width), ids)
    high, low = call(
        functools.partial(route_kernel, per_chunk),
        [shape(tokens, experts * capacity)] * 2,
        [VMEM, VMEM],
        2 * 2 * rows * tokens * part,
        12,
    )(ids, route_weight.T)
    weights = (gate_weight[0], up_weight[0], down_weight[0])
    whole, halves = shape(rows, part), shape(half, part)

    def run(chunk, outs, blocks):
        return call(
            functools.partial(expert_kernel, chunk),
            outs,
            [SMEM] + [VMEM] * len(blocks) + [ANY] * 3,
            6 * rows * width * gate_weight.shape[2],
            50,
            [pltpu.VMEM(w.shape, bf16) for w in weights]
            + [pltpu.VMEM((rows, part), bf16)] * 3
            + [pltpu.SemaphoreType.DMA((2 * count + 1,))],
        )(tp, *blocks, *weights)

    def fold(kernel, kind, *terms):
        return call(kernel, [kind] * 2, [VMEM] * 4, 10**8, 8)(*terms)

    def total(kernel, *terms):
        return call(kernel, whole, [VMEM] * len(terms), 10**8, 8)(*terms)

    arrived = exchange(sent[0])
    others = gather_direct(arrived)
    own, ahead, behind, top, bottom = run(0, [whole] * 3 + [halves] * 2, (arrived, *others))
    top = over_tp(top, 1)
    bottom = over_tp(bottom, -1)
    ahead, behind = fold(fold_whole_kernel, whole, ahead, top, behind, bottom)
    ahead = over_tp(ahead, 1)
    behind = over_tp(behind, -1)
    answer = total(total_whole_kernel, own, ahead, behind)
    answers = [exchange(answer)]
    arrived = exchange(sent[1])
    others = gather_relayed(arrived)
    own, ahead0, ahead1, behind0, behind1, across0, across1 = run(
        1, [whole] + [halves] * 6, (arrived, *others)
    )
    across0 = over_tp(across0, 1)
    across1 = over_tp(across1, -1)
    bottom0 = over_tp(ahead1, 1)
    top0 = over_tp(behind0, -1)
    ahead0, behind1 = fold(fold_kernel, halves, ahead0, across0, behind1, across1)
    top1 = over_tp(ahead0, 1)
    bottom1 = over_tp(behind1, -1)
    answer = total(total_kernel, own, top0, top1, bottom0, bottom1)
    answers.append(exchange(answer))
    return call(
        combine_kernel,
        shape(tokens, part),
        [VMEM, VMEM, ANY, ANY],
        4 * tokens * rows * part,
        56,
        [pltpu.VMEM((rows, part), bf16)] * 2 + [pltpu.SemaphoreType.DMA((2,))],
    )(high, low, *answers)


def on_device(
    glu_value,
    glu_gate,
    conv_kernel,
    ln_gain,
    out_weight,
    moe_input,
    moe_gain,
    gate_weight,
    up_weight,
    down_weight,
    expert_ids,
    route_weight,
):
    mixer_out = mixer_half(glu_value, glu_gate, conv_kernel, ln_gain, out_weight)
    expert_out = expert_half(
        moe_input, moe_gain, gate_weight, up_weight, down_weight, expert_ids, route_weight
    )
    return (mixer_out, expert_out)


def solution(mesh):
    in_specs = (
        P("ep", "tp"),
        P("ep", "tp"),
        P(None, "tp"),
        P("tp"),
        P("tp", None),
        P("ep", None),
        P(),
        P("ep", None, "tp"),
        P("ep", None, "tp"),
        P("ep", "tp", None),
        P("ep", None),
        P("ep", None),
    )
    out_specs = (P(("ep", "tp"), None), P("ep", "tp"))

    return jax.shard_map(on_device, mesh=mesh, in_specs=in_specs, out_specs=out_specs, check_vma=False)
```

```python
import functools

import jax
import jax.numpy as jnp
from jax import lax
from jax.experimental import pallas as pl
from jax.experimental.pallas import tpu as pltpu
from jax.sharding import PartitionSpec as P


eps_rms = 1e-06
eps_norm = 1e-05
f32 = jnp.float32
bf16 = jnp.bfloat16


VMEM = pl.BlockSpec(memory_space=pltpu.VMEM)
SMEM = pl.BlockSpec(memory_space=pltpu.SMEM)
ANY = pl.BlockSpec(memory_space=pl.ANY)


def dot(a, b):
    return jnp.dot(a, b, preferred_element_type=f32)


def over_tp(value, by):
    count = lax.axis_size("tp")
    return lax.ppermute(value, "tp", [(i, (i + by) % count) for i in range(count)])


def from_behind(value, axis, by):
    count = lax.axis_size(axis)
    return lax.ppermute(value, axis, [(i, i + by) for i in range(count - by)])


def swap_cores(value):
    count = lax.axis_size("ep")
    return lax.ppermute(value, "ep", [(i, i ^ 1) for i in range(count)])


def gather_direct(value):
    return over_tp(value, -1), over_tp(value, 1), over_tp(value, 2)


def gather_relayed(value):
    half = value.shape[0] // 2
    ahead = over_tp(value, -1)
    behind = over_tp(value, 1)
    top = over_tp(ahead[:half], -1)
    bottom = over_tp(behind[half:], 1)
    return ahead, behind, top, bottom


def slot_tables(ids, rows, tokens, per_chunk):
    expert_of = lax.broadcasted_iota(jnp.int32, (rows, tokens), 0) // per_chunk
    first = expert_of == ids[0:1, :]
    second = expert_of == ids[1:2, :]
    chosen = jnp.logical_or(first, second)
    before = (
        lax.broadcasted_iota(jnp.int32, (tokens, tokens), 0)
        < lax.broadcasted_iota(jnp.int32, (tokens, tokens), 1)
    ).astype(f32).astype(bf16)
    earlier = dot(chosen.astype(f32).astype(bf16), before).astype(jnp.int32)
    place = lax.broadcasted_iota(jnp.int32, (rows, tokens), 0) % per_chunk
    return first, second, chosen, earlier, place


def fetch(sources, targets, sems):
    copies = [
        pltpu.make_async_copy(source, target, sems.at[i])
        for i, (source, target) in enumerate(zip(sources, targets))
    ]
    for copy in copies:
        copy.start()
    return copies


def dispatch_kernel(per_chunk, tp_ref, x_hbm, gain_hbm, ids_hbm, o0, o1, x_ref, gain_ref, ids_ref, sems):
    outs = (o0, o1)
    tokens, width = x_ref.shape
    rows, part = o0.shape
    ids_copy, x_copy, gain_copy = fetch(
        (ids_hbm, x_hbm, gain_hbm), (ids_ref, x_ref, gain_ref), sems
    )
    ids_copy.wait()
    _, _, chosen, earlier, place = slot_tables(ids_ref[...], rows, tokens, per_chunk)
    picks = [
        jnp.logical_and(chosen, earlier == place + chunk * per_chunk).astype(f32).astype(bf16)
        for chunk in range(len(outs))
    ]
    x_copy.wait()
    gain_copy.wait()
    squares = jnp.zeros((tokens, 128), f32)
    for begin in range(0, width, 128):
        block = x_ref[:, begin : begin + 128].astype(f32)
        squares = squares + block * block
    scale = lax.rsqrt(jnp.sum(squares, axis=1, keepdims=True) / width + eps_rms)
    start = pl.multiple_of(tp_ref[0] * part, part)
    mine = x_ref[:, pl.ds(start, part)].astype(f32)
    normed = (mine * scale * gain_ref[:, pl.ds(start, part)]).astype(bf16)
    for pick, out in zip(picks, outs):
        out[...] = dot(pick, normed).astype(bf16)


def route_kernel(per_chunk, ids_ref, weight_ref, high_ref, low_ref):
    tokens, slots = high_ref.shape
    rows = slots // 2
    first, second, _, earlier, place = slot_tables(ids_ref[...], rows, tokens, per_chunk)
    amount = jnp.where(first, weight_ref[0:1, :], jnp.where(second, weight_ref[1:2, :], 0.0))
    for chunk in range(2):
        weights = jnp.where(earlier == place + chunk * per_chunk, amount, 0.0).T
        high = weights.astype(bf16)
        high_ref[:, chunk * rows : (chunk + 1) * rows] = high
        low_ref[:, chunk * rows : (chunk + 1) * rows] = (weights - high.astype(f32)).astype(bf16)


def rows_of_blocks(tp, part, count):
    return [pl.multiple_of(lax.rem(tp + k, count) * part, part) for k in (0, 1, count - 1, 2)]


def expert_rows(at, blocks, starts, gate_ref, up_ref, down_ref, outs, arrive):
    part = blocks[0].shape[1]
    gate = None
    up = None
    for k, (x, start) in enumerate(zip(blocks, starts)):
        arrive(k)
        block = x[at, :]
        g = dot(block, gate_ref[pl.ds(start, part), :])
        u = dot(block, up_ref[pl.ds(start, part), :])
        gate = g if gate is None else gate + g
        up = u if up is None else up + u
    hidden = (jax.nn.silu(gate) * up).astype(bf16)
    arrive(len(blocks))
    for out, start in zip(outs, starts):
        out[at, :] = dot(hidden, down_ref[:, pl.ds(start, part)]).astype(bf16)


def first_expert_kernel(
    tp_ref, x0, x1, x2, x3, gate_hbm, up_hbm, down_hbm,
    to_own, to_ahead, to_behind, across_top, across_bottom, gate_ref, up_ref, down_ref,
    own, ahead, behind, across_in, across, sems,
):
    rows, part = own.shape
    half = rows // 2
    blocks = (own, ahead, behind, across_in)
    starts = rows_of_blocks(tp_ref[0], part, gate_ref.shape[0] // part)
    sources, targets = [], []
    for hbm, block, start in zip((x0, x1, x2, x3), blocks, starts):
        at = pl.ds(start, part)
        sources += [hbm, gate_hbm.at[at, :], up_hbm.at[at, :]]
        targets += [block, gate_ref.at[at, :], up_ref.at[at, :]]
    depth = down_ref.shape[0] // 3
    for k in range(3):
        at = pl.ds(k * depth, depth)
        sources.append(down_hbm.at[at, :])
        targets.append(down_ref.at[at, :])
    copies = fetch(sources, targets, sems)

    def arrive(k):
        for copy in copies[3 * k : 3 * k + 3]:
            copy.wait()

    outs = (to_own, to_ahead, to_behind, across)
    expert_rows(pl.ds(0, half), blocks, starts, gate_ref, up_ref, down_ref, outs, arrive)
    expert_rows(
        pl.ds(half, half), blocks, starts, gate_ref, up_ref, down_ref, outs, lambda k: None
    )
    across_top[...] = across[:half, :]
    across_bottom[...] = across[half:, :]


def second_expert_kernel(
    tp_ref, own, ahead, behind, top, bottom, gate_ref, up_ref, down_ref,
    to_own, ahead_top, ahead_bottom, behind_top, behind_bottom, across_top, across_bottom,
    across, to_ahead, to_behind,
):
    rows, part = own.shape
    half = rows // 2
    across[:half, :] = top[...]
    across[half:, :] = bottom[...]
    blocks = (own, ahead, behind, across)
    starts = rows_of_blocks(tp_ref[0], part, gate_ref.shape[0] // part)

    def step(i, carry):
        at = pl.ds(pl.multiple_of(i * half, half), half)
        outs = (to_own, to_ahead, to_behind, across)
        expert_rows(at, blocks, starts, gate_ref, up_ref, down_ref, outs, lambda k: None)
        return carry

    lax.fori_loop(0, 2, step, 0)
    for source, upper, lower in (
        (across, across_top, across_bottom),
        (to_ahead, ahead_top, ahead_bottom),
        (to_behind, behind_top, behind_bottom),
    ):
        upper[...] = source[:half, :]
        lower[...] = source[half:, :]


def fold_kernel(ahead, top, behind, bottom, ahead_out, behind_out):
    half = top.shape[0]
    ahead_out[:half, :] = (ahead[:half, :].astype(f32) + top[...].astype(f32)).astype(bf16)
    ahead_out[half:, :] = ahead[half:, :]
    behind_out[:half, :] = behind[:half, :]
    behind_out[half:, :] = (behind[half:, :].astype(f32) + bottom[...].astype(f32)).astype(bf16)


def total_kernel(*refs):
    out = refs[-1]
    out[...] = sum(term[...].astype(f32) for term in refs[:-1]).astype(bf16)


def total_halves_kernel(own, top0, top1, bottom0, bottom1, out, *scratch):
    half = top0.shape[0]
    copies = fetch((own, top0, bottom0, top1, bottom1), scratch[:5], scratch[5])
    for copy in copies:
        copy.wait()
    own, top0, bottom0, top1, bottom1 = (ref[...].astype(f32) for ref in scratch[:5])
    out[:half, :] = (own[:half, :] + top0 + top1).astype(bf16)
    out[half:, :] = (own[half:, :] + bottom0 + bottom1).astype(bf16)


def fold_halves_kernel(a, b, c, d, ab, cd):
    ab[...] = (a[...].astype(f32) + b[...].astype(f32)).astype(bf16)
    cd[...] = (c[...].astype(f32) + d[...].astype(f32)).astype(bf16)


def conv_kernel_body(reach, halo, b0, b1, b2, b3, out_ref, wide, kept):
    own = out_ref.shape[0]
    part = b0.shape[1]
    channels = 4 * part
    total = jnp.zeros((own, 128), f32)
    square = jnp.zeros((own, 128), f32)
    rows = own + halo
    gains = []
    for k, block in enumerate((b0, b1, b2, b3)):
        taps = sum(
            block[rows + i * (reach + 1) : rows + (i + 1) * (reach + 1), :].astype(f32)
            for i in range(3)
        )
        gains.append(taps[reach : reach + 1, :])
        for begin in range(0, part, 128):
            lanes = slice(begin, begin + 128)
            wide[...] = block[:rows, lanes].astype(f32)
            value = jnp.zeros((own, 128), f32)
            for j in range(reach):
                value = value + taps[j : j + 1, lanes] * wide[halo - j : halo - j + own, :]
            kept[:, k * part + begin : k * part + begin + 128] = value
            total = total + value
            square = square + value * value
    mean = jnp.sum(total, axis=1, keepdims=True) / channels
    variance = jnp.sum(square, axis=1, keepdims=True) / channels - mean * mean
    scale = lax.rsqrt(variance + eps_norm)
    for k in range(4):
        lanes = slice(k * part, (k + 1) * part)
        scaled = (kept[:, lanes] - mean) * scale * gains[k]
        out_ref[:, lanes] = jax.nn.silu(scaled).astype(bf16)


def mix_kernel(core_ref, act, own, n1, n2, n3, f12, f3, out_ref):
    part = own.shape[0]
    columns = n1.shape[1]
    core = core_ref[0]
    near_at = pl.ds(pl.multiple_of(core * columns, columns), columns)
    far_at = pl.ds(pl.multiple_of((1 - core) * columns, columns), columns)
    cut = lambda k, n=1: act[:, k * part : (k + n) * part]
    near = dot(cut(0), own[:, near_at]) + dot(cut(1), n1[...])
    near = near + dot(cut(2), n2[...]) + dot(cut(3), n3[...])
    out_ref[:, near_at] = near.astype(bf16)
    far = dot(cut(0), own[:, far_at]) + dot(cut(1, 2), f12[...]) + dot(cut(3), f3[...])
    out_ref[:, far_at] = far.astype(bf16)


def combine_kernel(high_hbm, low_hbm, a0_hbm, a1_hbm, out_ref, high_ref, low_ref, a0, a1, sems):
    rows = a0.shape[0]
    copies = fetch(
        (high_hbm, a0_hbm, low_hbm, a1_hbm), (high_ref, a0, low_ref, a1), sems
    )
    for copy in copies[:3]:
        copy.wait()
    total = dot(high_ref[:, :rows], a0[...]) + dot(low_ref[:, :rows], a0[...])
    copies[3].wait()
    total = total + dot(high_ref[:, rows:], a1[...]) + dot(low_ref[:, rows:], a1[...])
    out_ref[...] = total.astype(bf16)


def call(kernel, out_shape, in_specs, flops, limit, scratch=()):
    many = isinstance(out_shape, (list, tuple))
    return pl.pallas_call(
        kernel,
        out_shape=out_shape,
        in_specs=in_specs,
        out_specs=[VMEM] * len(out_shape) if many else VMEM,
        scratch_shapes=scratch,
        compiler_params=pltpu.CompilerParams(vmem_limit_bytes=limit * 1024 * 1024),
        cost_estimate=pl.CostEstimate(flops=flops, bytes_accessed=1 << 20, transcendentals=0),
    )


def shape(*dims):
    return jax.ShapeDtypeStruct(dims, bf16)


def split_three(value):
    high = value.astype(bf16)
    rest = value - high.astype(f32)
    middle = rest.astype(bf16)
    return high, middle, (rest - middle.astype(f32)).astype(bf16)


def mixer_half(glu_value, glu_gate, conv_kernel, ln_gain, out_weight):
    tp = lax.axis_index("tp")
    core = lax.axis_index("ep") % 2
    length, part = glu_value.shape
    reach = conv_kernel.shape[0]
    count = lax.axis_size("tp")
    own = length // count
    halo = 32
    columns = out_weight.shape[1] // 2
    mine = lax.dynamic_slice_in_dim(out_weight, core * columns, columns, 1)
    near = [over_tp(mine, -1), over_tp(mine, 1)]
    far = [swap_cores(jnp.concatenate(near, axis=0))]
    near.append(over_tp(mine, 2))
    far.append(swap_cores(near[2]))
    taps = jnp.concatenate([conv_kernel, ln_gain[None, :]], axis=0)
    taps = split_three(taps)
    gated = (glu_value.astype(f32) * jax.nn.sigmoid(glu_gate.astype(f32))).astype(bf16)
    before = from_behind(gated[length - halo :], "ep", 1)
    padded = jnp.concatenate([before, gated], axis=0)

    def rows_of(k):
        rows = lax.dynamic_slice_in_dim(padded, ((tp + k) % count) * own, own + halo, 0)
        return jnp.concatenate([rows, *taps], axis=0)

    blocks = (
        rows_of(0),
        over_tp(rows_of(count - 1), -1),
        over_tp(rows_of(1), 1),
        over_tp(rows_of(2), 2),
    )
    activated = call(
        functools.partial(conv_kernel_body, reach, halo),
        shape(own, part * count),
        [VMEM] * 4,
        10**9,
        8,
        [pltpu.VMEM((own + halo, 128), f32), pltpu.VMEM((own, part * count), f32)],
    )(*blocks)
    return call(
        mix_kernel,
        shape(own, 2 * columns),
        [SMEM] + [VMEM] * 7,
        2 * own * part * count * 2 * columns,
        8,
    )(core.astype(jnp.int32).reshape(1), activated, out_weight, *near, *far)


def expert_half(moe_input, moe_gain, gate_weight, up_weight, down_weight, expert_ids, route_weight):
    tokens, width = moe_input.shape
    experts = lax.axis_size("ep")
    count = lax.axis_size("tp")
    capacity = 4 * max(1, tokens // experts)
    chunks = 2
    per_chunk = capacity // chunks
    rows = experts * per_chunk
    half = rows // 2
    part = width // count
    tp = lax.axis_index("tp").astype(jnp.int32).reshape(1)
    ids = expert_ids.T

    def exchange(value):
        value = value.reshape(experts, per_chunk, part)
        moved = lax.all_to_all(value, "ep", split_axis=0, concat_axis=0, tiled=True)
        return moved.reshape(rows, part)

    sent = call(
        functools.partial(dispatch_kernel, per_chunk),
        [shape(rows, part)] * chunks,
        [SMEM, ANY, ANY, ANY],
        2 * 2 * rows * tokens * part,
        56,
        [
            pltpu.VMEM((tokens, width), bf16),
            pltpu.VMEM((1, width), f32),
            pltpu.VMEM(ids.shape, jnp.int32),
            pltpu.SemaphoreType.DMA((3,)),
        ],
    )(tp, moe_input, moe_gain.reshape(1, width), ids)
    high, low = call(
        functools.partial(route_kernel, per_chunk),
        [shape(tokens, experts * capacity)] * 2,
        [VMEM, VMEM],
        2 * 2 * rows * tokens * part,
        12,
    )(ids, route_weight.T)
    weights = (gate_weight[0], up_weight[0], down_weight[0])
    whole, halves = shape(rows, part), shape(half, part)
    flops = 6 * rows * width * gate_weight.shape[2]
    vmem_blocks = [pltpu.VMEM((rows, part), bf16)]

    def total(*terms):
        return call(total_kernel, whole, [VMEM] * len(terms), 10**8, 8)(*terms)

    arrived = exchange(sent[0])
    others = gather_direct(arrived)
    own, ahead, behind, top, bottom, *weights = call(
        first_expert_kernel,
        [whole] * 3 + [halves] * 2 + [shape(*w.shape) for w in weights],
        [SMEM] + [ANY] * 7,
        flops,
        39,
        vmem_blocks * 5 + [pltpu.SemaphoreType.DMA((3 * count + 3,))],
    )(tp, arrived, *others, *weights)
    top = over_tp(top, 1)
    bottom = over_tp(bottom, -1)
    ahead, behind = call(fold_kernel, [whole] * 2, [VMEM] * 4, 10**8, 8)(ahead, top, behind, bottom)
    ahead = over_tp(ahead, 1)
    behind = over_tp(behind, -1)
    answer = total(own, ahead, behind)
    answers = [exchange(answer)]
    arrived = exchange(sent[1])
    others = gather_relayed(arrived)
    own, ahead0, ahead1, behind0, behind1, across0, across1 = call(
        second_expert_kernel,
        [whole] + [halves] * 6,
        [SMEM] + [VMEM] * 8,
        flops,
        16,
        vmem_blocks * 3,
    )(tp, arrived, *others, *weights)
    across0 = over_tp(across0, 1)
    across1 = over_tp(across1, -1)
    bottom0 = over_tp(ahead1, 1)
    top0 = over_tp(behind0, -1)
    ahead0, behind1 = call(
        fold_halves_kernel, [halves] * 2, [VMEM] * 4, 10**8, 8
    )(ahead0, across0, behind1, across1)
    top1 = over_tp(ahead0, 1)
    bottom1 = over_tp(behind1, -1)
    answer = call(
        total_halves_kernel,
        whole,
        [ANY] * 5,
        10**8,
        56,
        vmem_blocks + [pltpu.VMEM((half, part), bf16)] * 4 + [pltpu.SemaphoreType.DMA((5,))],
    )(own, top0, top1, bottom0, bottom1)
    answers.append(exchange(answer))
    return call(
        combine_kernel,
        shape(tokens, part),
        [ANY] * 4,
        4 * tokens * rows * part,
        56,
        [pltpu.VMEM((tokens, experts * capacity), bf16)] * 2
        + vmem_blocks * 2
        + [pltpu.SemaphoreType.DMA((4,))],
    )(high, low, *answers)


def on_device(
    glu_value,
    glu_gate,
    conv_kernel,
    ln_gain,
    out_weight,
    moe_input,
    moe_gain,
    gate_weight,
    up_weight,
    down_weight,
    expert_ids,
    route_weight,
):
    mixer_out = mixer_half(glu_value, glu_gate, conv_kernel, ln_gain, out_weight)
    expert_out = expert_half(
        moe_input, moe_gain, gate_weight, up_weight, down_weight, expert_ids, route_weight
    )
    return (mixer_out, expert_out)


def solution(mesh):
    in_specs = (
        P("ep", "tp"),
        P("ep", "tp"),
        P(None, "tp"),
        P("tp"),
        P("tp", None),
        P("ep", None),
        P(),
        P("ep", None, "tp"),
        P("ep", None, "tp"),
        P("ep", "tp", None),
        P("ep", None),
        P("ep", None),
    )
    out_specs = (P(("ep", "tp"), None), P("ep", "tp"))

    return jax.shard_map(on_device, mesh=mesh, in_specs=in_specs, out_specs=out_specs, check_vma=False)
```

```python
import functools

import jax
import jax.numpy as jnp
from jax import lax
from jax.experimental import pallas as pl
from jax.experimental.pallas import tpu as pltpu
from jax.sharding import PartitionSpec as P


eps_rms = 1e-06
eps_norm = 1e-05
f32 = jnp.float32
bf16 = jnp.bfloat16


VMEM = pl.BlockSpec(memory_space=pltpu.VMEM)
SMEM = pl.BlockSpec(memory_space=pltpu.SMEM)
ANY = pl.BlockSpec(memory_space=pl.ANY)


def dot(a, b):
    return jnp.dot(a, b, preferred_element_type=f32)


def over_tp(value, by):
    count = lax.axis_size("tp")
    return lax.ppermute(value, "tp", [(i, (i + by) % count) for i in range(count)])


def from_behind(value, axis, by):
    count = lax.axis_size(axis)
    return lax.ppermute(value, axis, [(i, i + by) for i in range(count - by)])


def swap_cores(value):
    count = lax.axis_size("ep")
    return lax.ppermute(value, "ep", [(i, i ^ 1) for i in range(count)])


def gather_relayed(value):
    half = value.shape[0] // 2
    ahead = over_tp(value, -1)
    behind = over_tp(value, 1)
    top = over_tp(ahead[:half], -1)
    bottom = over_tp(behind[half:], 1)
    return ahead, behind, top, bottom


def slot_tables(ids, rows, tokens, per_chunk):
    expert_of = lax.broadcasted_iota(jnp.int32, (rows, tokens), 0) // per_chunk
    first = expert_of == ids[0:1, :]
    second = expert_of == ids[1:2, :]
    chosen = jnp.logical_or(first, second)
    before = (
        lax.broadcasted_iota(jnp.int32, (tokens, tokens), 0)
        < lax.broadcasted_iota(jnp.int32, (tokens, tokens), 1)
    ).astype(f32).astype(bf16)
    earlier = dot(chosen.astype(f32).astype(bf16), before).astype(jnp.int32)
    place = lax.broadcasted_iota(jnp.int32, (rows, tokens), 0) % per_chunk
    return first, second, chosen, earlier, place


def fetch(sources, targets, sems):
    copies = [
        pltpu.make_async_copy(source, target, sems.at[i])
        for i, (source, target) in enumerate(zip(sources, targets))
    ]
    for copy in copies:
        copy.start()
    return copies


def dispatch_kernel(per_chunk, tp_ref, x_hbm, gain_hbm, ids_hbm, o0, o1, x_ref, gain_ref, ids_ref, sems):
    outs = (o0, o1)
    tokens, width = x_ref.shape
    rows, part = o0.shape
    ids_copy, x_copy, gain_copy = fetch(
        (ids_hbm, x_hbm, gain_hbm), (ids_ref, x_ref, gain_ref), sems
    )
    ids_copy.wait()
    _, _, chosen, earlier, place = slot_tables(ids_ref[...], rows, tokens, per_chunk)
    picks = [
        jnp.logical_and(chosen, earlier == place + chunk * per_chunk).astype(f32).astype(bf16)
        for chunk in range(len(outs))
    ]
    x_copy.wait()
    gain_copy.wait()
    squares = jnp.zeros((tokens, 128), f32)
    for begin in range(0, width, 128):
        block = x_ref[:, begin : begin + 128].astype(f32)
        squares = squares + block * block
    scale = lax.rsqrt(jnp.sum(squares, axis=1, keepdims=True) / width + eps_rms)
    start = pl.multiple_of(tp_ref[0] * part, part)
    mine = x_ref[:, pl.ds(start, part)].astype(f32)
    normed = (mine * scale * gain_ref[:, pl.ds(start, part)]).astype(bf16)
    for pick, out in zip(picks, outs):
        out[...] = dot(pick, normed).astype(bf16)


def route_kernel(per_chunk, ids_ref, weight_ref, high_ref, low_ref):
    tokens, slots = high_ref.shape
    rows = slots // 2
    first, second, _, earlier, place = slot_tables(ids_ref[...], rows, tokens, per_chunk)
    amount = jnp.where(first, weight_ref[0:1, :], jnp.where(second, weight_ref[1:2, :], 0.0))
    for chunk in range(2):
        weights = jnp.where(earlier == place + chunk * per_chunk, amount, 0.0).T
        high = weights.astype(bf16)
        high_ref[:, chunk * rows : (chunk + 1) * rows] = high
        low_ref[:, chunk * rows : (chunk + 1) * rows] = (weights - high.astype(f32)).astype(bf16)


def rows_of_blocks(tp, part, count):
    return [pl.multiple_of(lax.rem(tp + k, count) * part, part) for k in (0, 1, count - 1, 2)]


def expert_rows(at, blocks, starts, gate_ref, up_ref, down_ref, outs, arrive):
    part = blocks[0].shape[1]
    gate = None
    up = None
    for k, (x, start) in enumerate(zip(blocks, starts)):
        arrive(k)
        block = x[at, :]
        g = dot(block, gate_ref[pl.ds(start, part), :])
        u = dot(block, up_ref[pl.ds(start, part), :])
        gate = g if gate is None else gate + g
        up = u if up is None else up + u
    hidden = (jax.nn.silu(gate) * up).astype(bf16)
    arrive(len(blocks))
    for out, start in zip(outs, starts):
        out[at, :] = dot(hidden, down_ref[:, pl.ds(start, part)]).astype(bf16)


def first_expert_kernel(
    tp_ref, x0, x1, x2, x3, gate_hbm, up_hbm, down_hbm,
    to_own, to_ahead, to_behind, across_top, across_bottom, gate_ref, up_ref, down_ref,
    own, ahead, behind, across_in, across, sems,
):
    rows, part = own.shape
    half = rows // 2
    blocks = (own, ahead, behind, across_in)
    starts = rows_of_blocks(tp_ref[0], part, gate_ref.shape[0] // part)
    sources, targets = [], []
    for hbm, block, start in zip((x0, x1, x2, x3), blocks, starts):
        at = pl.ds(start, part)
        sources += [hbm, gate_hbm.at[at, :], up_hbm.at[at, :]]
        targets += [block, gate_ref.at[at, :], up_ref.at[at, :]]
    depth = down_ref.shape[0] // 3
    for k in range(3):
        at = pl.ds(k * depth, depth)
        sources.append(down_hbm.at[at, :])
        targets.append(down_ref.at[at, :])
    copies = fetch(sources, targets, sems)

    def arrive(k):
        for copy in copies[3 * k : 3 * k + 3]:
            copy.wait()

    outs = (to_own, to_ahead, to_behind, across)
    expert_rows(pl.ds(0, half), blocks, starts, gate_ref, up_ref, down_ref, outs, arrive)
    expert_rows(
        pl.ds(half, half), blocks, starts, gate_ref, up_ref, down_ref, outs, lambda k: None
    )
    across_top[...] = across[:half, :]
    across_bottom[...] = across[half:, :]


def second_expert_kernel(
    tp_ref, own, ahead, behind, top, bottom, gate_ref, up_ref, down_ref,
    to_own, to_ahead, to_behind, to_across, across,
):

    rows, part = own.shape
    half = rows // 2
    across[:half, :] = top[...]
    across[half:, :] = bottom[...]
    blocks = (own, ahead, behind, across)
    starts = rows_of_blocks(tp_ref[0], part, gate_ref.shape[0] // part)

    def step(i, carry):
        at = pl.ds(pl.multiple_of(i * half, half), half)
        outs = (to_own, to_ahead, to_behind, to_across)
        expert_rows(at, blocks, starts, gate_ref, up_ref, down_ref, outs, lambda k: None)
        return carry

    lax.fori_loop(0, 2, step, 0)


def fold_kernel(ahead, top, behind, bottom, ahead_out, behind_out):
    half = top.shape[0]
    ahead_out[:half, :] = (ahead[:half, :].astype(f32) + top[...].astype(f32)).astype(bf16)
    ahead_out[half:, :] = ahead[half:, :]
    behind_out[:half, :] = behind[:half, :]
    behind_out[half:, :] = (behind[half:, :].astype(f32) + bottom[...].astype(f32)).astype(bf16)


def total_kernel(*refs):
    out = refs[-1]
    out[...] = sum(term[...].astype(f32) for term in refs[:-1]).astype(bf16)


def total_fetched_kernel(h0, h1, h2, h3, out, v0, v1, v2, v3, sems):
    total = None
    values = (v0, v1, v2, v3)
    for copy, value in zip(fetch((h0, h1, h2, h3), values, sems), values):
        copy.wait()
        term = value[...].astype(f32)
        total = term if total is None else total + term
    out[...] = total.astype(bf16)


def conv_kernel_body(reach, halo, b0, b1, b2, b3, out_ref, wide, kept):
    own = out_ref.shape[0]
    part = b0.shape[1]
    channels = 4 * part
    total = jnp.zeros((own, 128), f32)
    square = jnp.zeros((own, 128), f32)
    rows = own + halo
    gains = []
    for k, block in enumerate((b0, b1, b2, b3)):
        taps = sum(
            block[rows + i * (reach + 1) : rows + (i + 1) * (reach + 1), :].astype(f32)
            for i in range(3)
        )
        gains.append(taps[reach : reach + 1, :])
        for begin in range(0, part, 128):
            lanes = slice(begin, begin + 128)
            wide[...] = block[:rows, lanes].astype(f32)
            value = jnp.zeros((own, 128), f32)
            for j in range(reach):
                value = value + taps[j : j + 1, lanes] * wide[halo - j : halo - j + own, :]
            kept[:, k * part + begin : k * part + begin + 128] = value
            total = total + value
            square = square + value * value
    mean = jnp.sum(total, axis=1, keepdims=True) / channels
    variance = jnp.sum(square, axis=1, keepdims=True) / channels - mean * mean
    scale = lax.rsqrt(variance + eps_norm)
    for k in range(4):
        lanes = slice(k * part, (k + 1) * part)
        scaled = (kept[:, lanes] - mean) * scale * gains[k]
        out_ref[:, lanes] = jax.nn.silu(scaled).astype(bf16)


def mix_kernel(core_ref, act, own, n1, n2, n3, n4, far_ref, out_ref):
    part = own.shape[0]
    columns = n1.shape[1]
    core = core_ref[0]
    near_at = pl.ds(pl.multiple_of(core * columns, columns), columns)
    far_at = pl.ds(pl.multiple_of((1 - core) * columns, columns), columns)
    cut = lambda k, n=1: act[:, k * part : (k + n) * part]
    near = dot(cut(0), own[:, near_at]) + dot(cut(1), n1[...]) + dot(cut(2), n2[...])
    near = near + dot(act[:, 3 * part : 3 * part + part // 2], n3[...])
    near = near + dot(act[:, 3 * part + part // 2 :], n4[...])
    out_ref[:, near_at] = near.astype(bf16)
    far = dot(cut(0), own[:, far_at]) + dot(cut(1, 3), far_ref[...])
    out_ref[:, far_at] = far.astype(bf16)


def combine_kernel(high_hbm, low_hbm, a0_hbm, a1_hbm, out_ref, high_ref, low_ref, a0, a1, sems):
    rows = a0.shape[0]
    copies = fetch(
        (high_hbm, a0_hbm, low_hbm, a1_hbm), (high_ref, a0, low_ref, a1), sems
    )
    for copy in copies[:3]:
        copy.wait()
    total = dot(high_ref[:, :rows], a0[...]) + dot(low_ref[:, :rows], a0[...])
    copies[3].wait()
    total = total + dot(high_ref[:, rows:], a1[...]) + dot(low_ref[:, rows:], a1[...])
    out_ref[...] = total.astype(bf16)


def call(kernel, out_shape, in_specs, flops, limit, scratch=()):
    many = isinstance(out_shape, (list, tuple))
    return pl.pallas_call(
        kernel,
        out_shape=out_shape,
        in_specs=in_specs,
        out_specs=[VMEM] * len(out_shape) if many else VMEM,
        scratch_shapes=scratch,
        compiler_params=pltpu.CompilerParams(vmem_limit_bytes=limit * 1024 * 1024),
        cost_estimate=pl.CostEstimate(flops=flops, bytes_accessed=1 << 20, transcendentals=0),
    )


def shape(*dims):
    return jax.ShapeDtypeStruct(dims, bf16)


def split_three(value):
    high = value.astype(bf16)
    rest = value - high.astype(f32)
    middle = rest.astype(bf16)
    return high, middle, (rest - middle.astype(f32)).astype(bf16)


def mixer_half(glu_value, glu_gate, conv_kernel, ln_gain, out_weight):
    tp = lax.axis_index("tp")
    core = lax.axis_index("ep") % 2
    length, part = glu_value.shape
    reach = conv_kernel.shape[0]
    count = lax.axis_size("tp")
    own = length // count
    halo = 32
    columns = out_weight.shape[1] // 2
    mine = lax.dynamic_slice_in_dim(out_weight, core * columns, columns, 1)
    near = [over_tp(mine, -1), over_tp(mine, 1)]
    near.append(over_tp(near[0][: part // 2], -1))
    near.append(over_tp(near[1][part // 2 :], 1))
    far = swap_cores(jnp.concatenate(near, axis=0))
    taps = jnp.concatenate([conv_kernel, ln_gain[None, :]], axis=0)
    taps = split_three(taps)
    gated = (glu_value.astype(f32) * jax.nn.sigmoid(glu_gate.astype(f32))).astype(bf16)
    before = from_behind(gated[length - halo :], "ep", 1)
    padded = jnp.concatenate([before, gated], axis=0)

    def rows_of(k):
        rows = lax.dynamic_slice_in_dim(padded, ((tp + k) % count) * own, own + halo, 0)
        return jnp.concatenate([rows, *taps], axis=0)

    blocks = (
        rows_of(0),
        over_tp(rows_of(count - 1), -1),
        over_tp(rows_of(1), 1),
        over_tp(rows_of(2), 2),
    )
    activated = call(
        functools.partial(conv_kernel_body, reach, halo),
        shape(own, part * count),
        [VMEM] * 4,
        10**9,
        8,
        [pltpu.VMEM((own + halo, 128), f32), pltpu.VMEM((own, part * count), f32)],
    )(*blocks)
    return call(
        mix_kernel,
        shape(own, 2 * columns),
        [SMEM] + [VMEM] * 7,
        2 * own * part * count * 2 * columns,
        8,
    )(core.astype(jnp.int32).reshape(1), activated, out_weight, *near, far)


def expert_half(moe_input, moe_gain, gate_weight, up_weight, down_weight, expert_ids, route_weight):
    tokens, width = moe_input.shape
    experts = lax.axis_size("ep")
    count = lax.axis_size("tp")
    capacity = 4 * max(1, tokens // experts)
    chunks = 2
    per_chunk = capacity // chunks
    rows = experts * per_chunk
    half = rows // 2
    part = width // count
    tp = lax.axis_index("tp").astype(jnp.int32).reshape(1)
    ids = expert_ids.T

    def exchange(value):
        value = value.reshape(experts, per_chunk, part)
        moved = lax.all_to_all(value, "ep", split_axis=0, concat_axis=0, tiled=True)
        return moved.reshape(rows, part)

    sent = call(
        functools.partial(dispatch_kernel, per_chunk),
        [shape(rows, part)] * chunks,
        [SMEM, ANY, ANY, ANY],
        2 * 2 * rows * tokens * part,
        56,
        [
            pltpu.VMEM((tokens, width), bf16),
            pltpu.VMEM((1, width), f32),
            pltpu.VMEM(ids.shape, jnp.int32),
            pltpu.SemaphoreType.DMA((3,)),
        ],
    )(tp, moe_input, moe_gain.reshape(1, width), ids)
    high, low = call(
        functools.partial(route_kernel, per_chunk),
        [shape(tokens, experts * capacity)] * 2,
        [VMEM, VMEM],
        2 * 2 * rows * tokens * part,
        12,
    )(ids, route_weight.T)
    weights = (gate_weight[0], up_weight[0], down_weight[0])
    whole, halves = shape(rows, part), shape(half, part)
    flops = 6 * rows * width * gate_weight.shape[2]
    vmem_blocks = [pltpu.VMEM((rows, part), bf16)]

    def total(*terms):
        return call(total_kernel, whole, [VMEM] * len(terms), 10**8, 8)(*terms)

    arrived = exchange(sent[0])
    others = [over_tp(arrived, -1), over_tp(arrived, 1)]
    others.append(over_tp(arrived, 2))
    own, ahead, behind, top, bottom, *weights = call(
        first_expert_kernel,
        [whole] * 3 + [halves] * 2 + [shape(*w.shape) for w in weights],
        [SMEM] + [ANY] * 7,
        flops,
        39,
        vmem_blocks * 5 + [pltpu.SemaphoreType.DMA((3 * count + 3,))],
    )(tp, arrived, *others, *weights)
    top = over_tp(top, 1)
    bottom = over_tp(bottom, -1)
    ahead, behind = call(fold_kernel, [whole] * 2, [VMEM] * 4, 10**8, 8)(ahead, top, behind, bottom)
    ahead = over_tp(ahead, 1)
    behind = over_tp(behind, -1)
    answer = total(own, ahead, behind)
    answers = [exchange(answer)]
    arrived = exchange(sent[1])
    others = gather_relayed(arrived)
    own, ahead, behind, across = call(
        second_expert_kernel, [whole] * 4, [SMEM] + [VMEM] * 8, flops, 16, vmem_blocks
    )(tp, arrived, *others, *weights)
    ahead = over_tp(ahead, 1)
    behind = over_tp(behind, -1)
    across = over_tp(across, 2)
    answer = call(
        total_fetched_kernel,
        whole,
        [ANY] * 4,
        10**8,
        56,
        vmem_blocks * 4 + [pltpu.SemaphoreType.DMA((4,))],
    )(own, ahead, behind, across)
    answers.append(exchange(answer))
    return call(
        combine_kernel,
        shape(tokens, part),
        [ANY] * 4,
        4 * tokens * rows * part,
        53,
        [pltpu.VMEM((tokens, experts * capacity), bf16)] * 2
        + vmem_blocks * 2
        + [pltpu.SemaphoreType.DMA((4,))],
    )(high, low, *answers)


def on_device(
    glu_value,
    glu_gate,
    conv_kernel,
    ln_gain,
    out_weight,
    moe_input,
    moe_gain,
    gate_weight,
    up_weight,
    down_weight,
    expert_ids,
    route_weight,
):
    mixer_out = mixer_half(glu_value, glu_gate, conv_kernel, ln_gain, out_weight)
    expert_out = expert_half(
        moe_input, moe_gain, gate_weight, up_weight, down_weight, expert_ids, route_weight
    )
    return (mixer_out, expert_out)


def solution(mesh):
    in_specs = (
        P("ep", "tp"),
        P("ep", "tp"),
        P(None, "tp"),
        P("tp"),
        P("tp", None),
        P("ep", None),
        P(),
        P("ep", None, "tp"),
        P("ep", None, "tp"),
        P("ep", "tp", None),
        P("ep", None),
        P("ep", None),
    )
    out_specs = (P(("ep", "tp"), None), P("ep", "tp"))

    return jax.shard_map(on_device, mesh=mesh, in_specs=in_specs, out_specs=out_specs, check_vma=False)
```
